32 devices in a mesh: dp: 4 (over y, x), kv: 4 (over z), tp: 2 (over core).
Axes of the slice: x: 2, y: 2, z: 4, core: 2. Of those that a mesh axis runs over, the one named last changes fastest.
Arguments:
- hidden: bfloat16 [2048, 16], P(('kv', 'tp'), 'dp'), parts along dimension 1, may hold values from -20 to 20
- mixer_gain: float32 [2048], replicated, may hold values from 0.1 to 1.9
- gate_proj: bfloat16 [2048, 64, 64], P(None, 'kv', 'tp'), may hold values from -0.125 to 0.125
- inner_proj: bfloat16 [2048, 64, 64], P(None, 'kv', 'tp'), may hold values from -0.125 to 0.125
- input_proj: bfloat16 [2048, 1024], P(None, 'kv'), may hold values from -0.125 to 0.125
- output_proj: bfloat16 [2048, 1024], P(None, 'kv'), may hold values from -0.125 to 0.125
- step_proj: bfloat16 [2048, 64], replicated, may hold values from -0.125 to 0.125
- step_bias: float32 [64], replicated, may hold values from -3 to -0.5
- decay_log: float32 [64], replicated, may hold values from -3 to 1
- skip_gain: float32 [64], replicated, may hold values from 0.3 to 1.5
- taps_inner: float32 [4, 64, 64], P(None, None, 'tp'), may hold values from -3 to 3
- taps_input: float32 [4, 1024], replicated, may hold values from -3 to 3
- taps_output: float32 [4, 1024], replicated, may hold values from -3 to 3
- recent_inner: bfloat16 [16, 3, 64, 64], P(('dp', 'kv'), None, None, 'tp'), parts along dimension 0, may hold values from -6 to 6
- recent_input: bfloat16 [16, 3, 1024], P(('dp', 'kv')), parts along dimension 0, may hold values from -6 to 6
- recent_output: bfloat16 [16, 3, 1024], P(('dp', 'kv')), parts along dimension 0, may hold values from -6 to 6
- states: float32 [16, 64, 64, 128], P(('dp', 'kv'), None, 'tp'), parts along dimension 0, may hold values from -4 to 4
- block_inner: bfloat16 [16, 128, 64, 64], P(('dp', 'kv'), None, None, 'tp'), parts along dimension 0, may hold values from -6 to 6
- block_input: bfloat16 [16, 128, 1024], P(('dp', 'kv')), parts along dimension 0, may hold values from -4 to 4
- block_decay: float32 [16, 128, 64], P(('dp', 'kv')), parts along dimension 0
- lengths: int32 [16], P(('dp', 'kv')), parts along dimension 0, may hold values from 1 to 128, 170 in all
- norm_gain: float32 [64, 64], P(None, 'tp'), may hold values from 0.1 to 1.9
- mixer_out: bfloat16 [64, 64, 2048], P('kv', 'tp'), may hold values from -0.125 to 0.125
- channel_gain: float32 [2048], replicated, may hold values from 0.1 to 1.9
- expand_gate: bfloat16 [2048, 5632], P(None, ('kv', 'tp')), may hold values from -0.125 to 0.125
- expand_value: bfloat16 [2048, 5632], P(None, ('kv', 'tp')), may hold values from -0.125 to 0.125
- reduce_proj: bfloat16 [5632, 2048], P(('kv', 'tp')), may hold values from -0.109375 to 0.109375
Outputs:
- layer_out: bfloat16 [2048, 16], P(('kv', 'tp'), 'dp'), parts along dimension 1
The draws below stay inside these ranges and needn't reach their ends.
There are 4 independent parts, one for each index of `dp`. The reference program is written for one: setup_inputs(seed, part) draws one part's arguments, and reference() takes and returns one part's arrays. A program takes and returns all parts, laid end to end along the dimension named above; an argument that names none is the same for every part. Nothing has to cross between parts.
All inputs are finite; a program needn't handle non-finite values. No bound on the sum of `lengths` on one device may be relied on, other than what follows from the above.
Results may differ from the reference program's by a relative error of at most 0.01.
Values may be sent and summed in bfloat16 or wider, within the bound.
A program may use at most 64 MiB of HBM per device.

```python
import math
import jax
import jax.numpy as jnp
import numpy as np
from jax import lax

D = 2048
MIXER_HEADS = 64
HEAD_DIM = 64
GROUPS = 8
STATE = 128
FF = 5632
TAPS = 4
OPEN_BLOCK_SPAN = 128
GROUP_SEQUENCES = 4


def draw_hidden(key, part):
    rows = jnp.arange(D, dtype=jnp.float32)[:, None] / D
    rising = 1.0 + 2.0 * rows
    base = jax.random.truncated_normal(key, -4.0, 4.0, (D, GROUP_SEQUENCES), jnp.float32)
    return (base * rising).astype(jnp.bfloat16)


def draw_block_decay(key, part):
    key_rate, key_seq, key_jitter, position_key, extent_key = jax.random.split(jax.random.fold_in(key, 17), 5)
    low, high = (math.log(0.2 / OPEN_BLOCK_SPAN), math.log(0.08))
    arrival_rate = jnp.exp(jax.random.uniform(key_rate, (1, 1, MIXER_HEADS), jnp.float32, low, high))
    sequence_share = jnp.exp(jax.random.uniform(key_seq, (GROUP_SEQUENCES, 1, 1), jnp.float32, math.log(0.5), math.log(2.0)))
    random_shift = jnp.exp(jax.random.uniform(key_jitter, (GROUP_SEQUENCES, OPEN_BLOCK_SPAN, MIXER_HEADS), jnp.float32, -0.35, 0.35))
    surge_position = (jax.random.randint(position_key, (GROUP_SEQUENCES, OPEN_BLOCK_SPAN, 1), 0, OPEN_BLOCK_SPAN) < 3).astype(jnp.float32)
    surge_extent = jax.random.uniform(extent_key, (GROUP_SEQUENCES, OPEN_BLOCK_SPAN, MIXER_HEADS), jnp.float32, 0.22, 0.69)
    return -(arrival_rate * sequence_share * random_shift) - surge_position * surge_extent


def raised(result, own_key, source, target, shards_of, factor):
    def block_of(position):
        return (jnp.arange(result.shape[position]) // (result.shape[position] // shards_of)).reshape((-1,) + (1,) * (result.ndim - 1 - position))

    one_side = jax.random.permutation(own_key, shards_of)[block_of(target)]
    other_side = (block_of(target) + shards_of // 2) % shards_of
    return jnp.where((block_of(source) == one_side) | (block_of(source) == other_side), factor * result, result)


def shard_levels(key, extent, shards, least, high):
    loudness = 1.0
    for position, shards_of in shards:
        draws = jax.random.uniform(jax.random.fold_in(jax.random.fold_in(key, 6), position), (shards_of,), jnp.float32, least / len(shards), high / len(shards))
        loudness = loudness * jnp.repeat(jnp.exp(draws), extent[position] // shards_of).reshape((-1,) + (1,) * (len(extent) - 1 - position))
    return loudness


def profile(count, total, reach, skew):
    portions = [(1 << 20) // math.isqrt(standing ** skew) + 1 for standing in range(2, count + 1)]
    rest, counts = total - reach - (count - 1), [1] * (count - 1)
    while rest > 0:
        movable = [i for i in range(count - 1) if counts[i] < reach]
        whole, budget = sum([portions[i] for i in movable]), rest
        for i in movable:
            extra = min(reach - counts[i], max(1, budget * portions[i] // whole), rest)
            counts[i] = counts[i] + extra
            rest = rest - extra
    return np.array([reach] + counts)


def uneven_parts(own_key, number_of, total, most, lean):
    if number_of == 2:
        one = jax.random.randint(own_key, (), max(1, total - most), min(most, total - 1) + 1)
        return jnp.stack([one, total - one])
    sizes = jnp.asarray(profile(number_of, total, most, lean), jnp.int32)
    pairs = (number_of - 1) // 2
    source_of, sink = sizes[1:1 + 2 * pairs:2], sizes[2:2 + 2 * pairs:2]
    room = jnp.minimum(source_of - 1, most - sink)
    moved = jax.random.randint(jax.random.fold_in(own_key, 1), (pairs,), 0, 1 << 20) % (room + 1)
    sizes = sizes.at[1:1 + 2 * pairs:2].set(source_of - moved).at[2:2 + 2 * pairs:2].set(sink + moved)
    return sizes[jax.random.permutation(jax.random.fold_in(own_key, 2), number_of)]


def centred(rng, shape, deviation, bound, cuts=(), kind=jnp.bfloat16):
    entries = deviation * jax.random.normal(rng, shape, jnp.float32)
    if cuts:
        entries = entries * shard_levels(rng, shape, cuts, -0.22, 0.18)
    return jnp.clip(entries, -bound, bound).astype(kind)


def bell_draw_with(stream_key, dims, width, reach, cuts, heavy, kind=jnp.bfloat16):
    array = width * jax.random.normal(stream_key, dims, jnp.float32)
    if cuts:
        array = array * shard_levels(stream_key, dims, cuts, -0.22, 0.18)
    return jnp.clip(raised(array, jax.random.fold_in(stream_key, 3), *heavy), -reach, reach).astype(kind)


def setup_inputs(seed: int = 0, part: int = 0) -> dict:
    seeds = jax.random.split(jax.random.key(seed), 28)
    part_keys = jax.random.split(jax.random.fold_in(seeds[27], part), 28)
    hidden = draw_hidden(jax.random.fold_in(jax.random.fold_in(seeds[27], part), 71), part)
    mixer_gain = jnp.clip(1.0 + 0.18 * jax.random.normal(seeds[1], (D,), jnp.float32), 0.1, 1.9)
    gate_proj = centred(seeds[2], (D, MIXER_HEADS, HEAD_DIM), D ** -0.5, 0.125, ((1, 4), (2, 2)))
    inner_proj = centred(seeds[3], (D, MIXER_HEADS, HEAD_DIM), D ** -0.5, 0.125, ((1, 4), (2, 2)))
    input_proj = centred(seeds[4], (D, GROUPS * STATE), D ** -0.5, 0.125, ((1, 4),))
    output_proj = centred(seeds[5], (D, GROUPS * STATE), D ** -0.5, 0.125, ((1, 4),))
    step_proj = centred(seeds[6], (D, MIXER_HEADS), D ** -0.5, 0.125)
    step_bias = jnp.clip(jax.random.uniform(seeds[7], (MIXER_HEADS,), jnp.float32, -3.0, -0.5), -3.0, -0.5)
    decay_log = jnp.clip(jax.random.uniform(seeds[8], (MIXER_HEADS,), jnp.float32, -3.0, 1.0), -3.0, 1.0)
    skip_gain = jnp.clip(jax.random.uniform(seeds[9], (MIXER_HEADS,), jnp.float32, 0.3, 1.5), 0.3, 1.5)
    taps_inner = centred(seeds[10], (TAPS, MIXER_HEADS, HEAD_DIM), TAPS ** -0.5, 3.0, ((2, 2),), jnp.float32)
    taps_input = centred(seeds[11], (TAPS, GROUPS * STATE), TAPS ** -0.5, 3.0, (), jnp.float32)
    taps_output = centred(seeds[12], (TAPS, GROUPS * STATE), TAPS ** -0.5, 3.0, (), jnp.float32)
    recent_inner = centred(part_keys[13], (GROUP_SEQUENCES, TAPS - 1, MIXER_HEADS, HEAD_DIM), 1.0, 6.0, ((0, 4), (3, 2)))
    recent_input = centred(part_keys[14], (GROUP_SEQUENCES, TAPS - 1, GROUPS * STATE), 1.0, 6.0, ((0, 4),))
    recent_output = centred(part_keys[15], (GROUP_SEQUENCES, TAPS - 1, GROUPS * STATE), 1.0, 6.0, ((0, 4),))
    states = centred(part_keys[16], (GROUP_SEQUENCES, MIXER_HEADS, HEAD_DIM, STATE), 0.3, 4.0, ((0, 4), (2, 2)), jnp.float32)
    block_inner = centred(part_keys[17], (GROUP_SEQUENCES, OPEN_BLOCK_SPAN, MIXER_HEADS, HEAD_DIM), 0.5, 6.0, ((0, 4), (3, 2)))
    block_input = centred(part_keys[18], (GROUP_SEQUENCES, OPEN_BLOCK_SPAN, GROUPS * STATE), 0.25, 4.0, ((0, 4),))
    block_decay = draw_block_decay(jax.random.fold_in(jax.random.fold_in(seeds[27], part), 71), part)
    lengths = uneven_parts(part_keys[20], GROUP_SEQUENCES, GROUP_SEQUENCES * OPEN_BLOCK_SPAN // 3, OPEN_BLOCK_SPAN, 2).astype(jnp.int32)
    norm_gain = jnp.clip(1.0 + 0.18 * jax.random.normal(seeds[21], (MIXER_HEADS, HEAD_DIM), jnp.float32), 0.1, 1.9)
    mixer_out = bell_draw_with(seeds[22], (MIXER_HEADS, HEAD_DIM, D), (MIXER_HEADS * HEAD_DIM) ** -0.5, 0.125, ((0, 4), (1, 2)), (0, 2, 4, 2.0))
    channel_gain = jnp.clip(1.0 + 0.18 * jax.random.normal(seeds[23], (D,), jnp.float32), 0.1, 1.9)
    expand_gate = centred(seeds[24], (D, FF), D ** -0.5, 0.125, ((1, 8),))
    expand_value = centred(seeds[25], (D, FF), D ** -0.5, 0.125, ((1, 8),))
    reduce_proj = bell_draw_with(seeds[26], (FF, D), FF ** -0.5, 0.109375, ((0, 8),), (0, 1, 8, 2.0))
    return {"hidden": hidden, "mixer_gain": mixer_gain, "gate_proj": gate_proj, "inner_proj": inner_proj, "input_proj": input_proj, "output_proj": output_proj, "step_proj": step_proj, "step_bias": step_bias, "decay_log": decay_log, "skip_gain": skip_gain, "taps_inner": taps_inner, "taps_input": taps_input, "taps_output": taps_output, "recent_inner": recent_inner, "recent_input": recent_input, "recent_output": recent_output, "states": states, "block_inner": block_inner, "block_input": block_input, "block_decay": block_decay, "lengths": lengths, "norm_gain": norm_gain, "mixer_out": mixer_out, "channel_gain": channel_gain, "expand_gate": expand_gate, "expand_value": expand_value, "reduce_proj": reduce_proj}


epsilon = 1e-05

def short_conv(recent, newest, taps):
    window = jnp.concatenate([recent.astype(jnp.float32), newest.astype(jnp.float32)[:, None]], axis=1)
    return jax.nn.silu(lax.optimization_barrier(jnp.sum(window * taps[None], axis=1)))

def reference(hidden, mixer_gain, gate_proj, inner_proj, input_proj, output_proj, step_proj, step_bias, decay_log, skip_gain, taps_inner, taps_input, taps_output, recent_inner, recent_input, recent_output, states, block_inner, block_input, block_decay, lengths, norm_gain, mixer_out, channel_gain, expand_gate, expand_value, reduce_proj):
    hidden_f = hidden.astype(jnp.float32)
    rms_in = lax.rsqrt(lax.optimization_barrier(jnp.mean(hidden_f * hidden_f, axis=0)) + epsilon)
    normed_in = (hidden_f * mixer_gain[:, None]).astype(jnp.bfloat16).astype(jnp.float32)
    gate_pre = (rms_in[:, None, None] * jnp.einsum('ds,dhp->shp', normed_in, gate_proj.astype(jnp.float32))).astype(jnp.bfloat16)
    inner_pre = (rms_in[:, None, None] * jnp.einsum('ds,dhp->shp', normed_in, inner_proj.astype(jnp.float32))).astype(jnp.bfloat16)
    input_pre = (rms_in[:, None] * jnp.einsum('ds,dk->sk', normed_in, input_proj.astype(jnp.float32))).astype(jnp.bfloat16)
    output_pre = (rms_in[:, None] * jnp.einsum('ds,dk->sk', normed_in, output_proj.astype(jnp.float32))).astype(jnp.bfloat16)
    step_pre = (rms_in[:, None] * jnp.einsum('ds,dh->sh', normed_in, step_proj.astype(jnp.float32))).astype(jnp.bfloat16)
    conv_inner = short_conv(recent_inner, inner_pre, taps_inner)
    conv_input = short_conv(recent_input, input_pre, taps_input)
    conv_output = short_conv(recent_output, output_pre, taps_output).astype(jnp.bfloat16)
    step = jax.nn.softplus(step_pre.astype(jnp.float32) + step_bias[None, :])
    new_decay = -jnp.exp(decay_log)[None, :] * step
    seq_count = hidden.shape[1]
    per_group = MIXER_HEADS // GROUPS
    live = (jnp.arange(OPEN_BLOCK_SPAN, dtype=jnp.int32)[None, :] < lengths[:, None]).astype(jnp.float32)
    masked = block_decay * live[:, :, None]
    cached = lax.optimization_barrier(jnp.sum(masked, axis=1))
    tail = new_decay[:, None, :] + cached[:, None, :] - jnp.cumsum(masked, axis=1)
    total = new_decay + cached
    readout = conv_output.astype(jnp.float32).reshape(seq_count, GROUPS, STATE)
    score = jnp.einsum('sgn,sjgn->sgj', readout, block_input.astype(jnp.float32).reshape(seq_count, OPEN_BLOCK_SPAN, GROUPS, STATE))
    score_heads = jnp.repeat(score, per_group, axis=1)
    weight = (live[:, None, :] * jnp.exp(jnp.swapaxes(tail, 1, 2)) * score_heads).astype(jnp.bfloat16)
    from_block = jnp.einsum('shj,sjhp->shp', weight.astype(jnp.float32), block_inner.astype(jnp.float32))
    grouped = states.reshape(seq_count, GROUPS, per_group, HEAD_DIM, STATE)
    from_state = jnp.einsum('sgn,sgrpn->sgrp', readout, grouped, precision=lax.Precision.HIGHEST).reshape(seq_count, MIXER_HEADS, HEAD_DIM)
    own_score = jnp.repeat(lax.optimization_barrier(jnp.sum(readout * conv_input.reshape(seq_count, GROUPS, STATE), axis=-1)), per_group, axis=1)
    mix = from_block + jnp.exp(total)[:, :, None] * from_state + (own_score * step)[:, :, None] * conv_inner + skip_gain[None, :, None] * conv_inner
    gated_raw = mix * jax.nn.silu(gate_pre.astype(jnp.float32))
    rms_gate = lax.rsqrt(lax.optimization_barrier(jnp.mean(gated_raw * gated_raw, axis=(1, 2))) + epsilon)
    gated = (gated_raw * norm_gain[None]).astype(jnp.bfloat16)
    mixed = rms_gate[None, :] * jnp.einsum('shp,hpd->ds', gated.astype(jnp.float32), mixer_out.astype(jnp.float32))
    mid = (hidden_f + mixed).astype(jnp.bfloat16).astype(jnp.float32)
    rms_mid = lax.rsqrt(lax.optimization_barrier(jnp.mean(mid * mid, axis=0)) + epsilon)
    normed_mid = (mid * channel_gain[:, None]).astype(jnp.bfloat16).astype(jnp.float32)
    gate_sum = rms_mid[:, None] * jnp.einsum('ds,df->sf', normed_mid, expand_gate.astype(jnp.float32))
    value_sum = rms_mid[:, None] * jnp.einsum('ds,df->sf', normed_mid, expand_value.astype(jnp.float32))
    act = (jax.nn.silu(gate_sum) * value_sum).astype(jnp.bfloat16)
    channel = jnp.einsum('fd,sf->ds', reduce_proj.astype(jnp.float32), act.astype(jnp.float32))
    return (mid + channel).astype(jnp.bfloat16)
```

```python
import jax
import jax.numpy as jnp
from jax import lax
from jax.sharding import PartitionSpec as P
from jax.experimental import pallas as pl
from jax.experimental.pallas import tpu as pltpu
import functools

MIXER_HEADS = 64
HEAD_DIM = 64
GROUPS = 8
STATE = 128
OPEN_BLOCK_SPAN = 128


epsilon = 1e-05


def short_conv(recent, newest, taps):
    window = jnp.concatenate(
        [recent.astype(jnp.float32), newest.astype(jnp.float32)[:, None]], axis=1
    )
    return jax.nn.silu(jnp.sum(window * taps[None], axis=1))


def shards(
    hidden,
    mixer_gain,
    gate_proj,
    inner_proj,
    input_proj,
    output_proj,
    step_proj,
    step_bias,
    decay_log,
    skip_gain,
    taps_inner,
    taps_input,
    taps_output,
    recent_inner,
    recent_input,
    recent_output,
    states,
    block_inner,
    block_input,
    block_decay,
    lengths,
    norm_gain,
    mixer_out,
    channel_gain,
    expand_gate,
    expand_value,
    reduce_proj,
):
    rows_own = hidden.shape[0]
    seq_all = hidden.shape[1]
    seq_dev = states.shape[0]
    half_dim = states.shape[2]
    width = rows_own * lax.axis_size("kv") * lax.axis_size("tp")
    offset = (lax.axis_index("kv") * lax.axis_size("tp") + lax.axis_index("tp")) * rows_own
    own_start = lax.axis_index("kv") * seq_dev
    whole_rows = lax.all_gather(hidden, ("kv", "tp"), axis=0, tiled=True)
    whole_f = whole_rows.astype(jnp.float32)
    rms_in = lax.rsqrt(jnp.mean(whole_f * whole_f, axis=0) + epsilon)
    normed_in = (whole_f * mixer_gain[:, None]).astype(jnp.bfloat16)
    gate_part = (
        rms_in[:, None, None]
        * jnp.einsum("ds,dhp->shp", normed_in, gate_proj, preferred_element_type=jnp.float32)
    ).astype(jnp.bfloat16)
    inner_part = (
        rms_in[:, None, None]
        * jnp.einsum("ds,dhp->shp", normed_in, inner_proj, preferred_element_type=jnp.float32)
    ).astype(jnp.bfloat16)
    input_part = (
        rms_in[:, None]
        * jnp.einsum("ds,dk->sk", normed_in, input_proj, preferred_element_type=jnp.float32)
    ).astype(jnp.bfloat16)
    output_part = (
        rms_in[:, None]
        * jnp.einsum("ds,dk->sk", normed_in, output_proj, preferred_element_type=jnp.float32)
    ).astype(jnp.bfloat16)
    own_cols = lax.dynamic_slice_in_dim(normed_in, own_start, seq_dev, 1)
    own_rms = lax.dynamic_slice_in_dim(rms_in, own_start, seq_dev, 0)
    step_pre = (
        own_rms[:, None]
        * jnp.einsum("ds,dh->sh", own_cols, step_proj, preferred_element_type=jnp.float32)
    ).astype(jnp.bfloat16)
    gate_pre, inner_pre, input_pre, output_pre = (
        lax.all_to_all(gate_part, "kv", split_axis=0, concat_axis=1, tiled=True),
        lax.all_to_all(inner_part, "kv", split_axis=0, concat_axis=1, tiled=True),
        lax.all_to_all(input_part, "kv", split_axis=0, concat_axis=1, tiled=True),
        lax.all_to_all(output_part, "kv", split_axis=0, concat_axis=1, tiled=True),
    )
    conv_inner = short_conv(recent_inner, inner_pre, taps_inner)
    conv_input = short_conv(recent_input, input_pre, taps_input)
    conv_output = short_conv(recent_output, output_pre, taps_output).astype(jnp.bfloat16)
    step = jax.nn.softplus(step_pre.astype(jnp.float32) + step_bias[None, :])
    new_decay = -jnp.exp(decay_log)[None, :] * step
    per_group = MIXER_HEADS // GROUPS
    live = (jnp.arange(OPEN_BLOCK_SPAN, dtype=jnp.int32)[None, :] < lengths[:, None]).astype(
        jnp.float32
    )
    masked = block_decay * live[:, :, None]
    cached = jnp.sum(masked, axis=1)
    tail = new_decay[:, None, :] + cached[:, None, :] - jnp.cumsum(masked, axis=1)
    total = new_decay + cached
    readout = conv_output.reshape(seq_dev, GROUPS, STATE)
    score = jnp.einsum(
        "sgn,sjgn->sgj",
        readout,
        block_input.reshape(seq_dev, OPEN_BLOCK_SPAN, GROUPS, STATE),
        preferred_element_type=jnp.float32,
    )
    score_heads = jnp.repeat(score, per_group, axis=1)
    weight = (live[:, None, :] * jnp.exp(jnp.swapaxes(tail, 1, 2)) * score_heads).astype(
        jnp.bfloat16
    )
    from_block = jnp.einsum(
        "shj,sjhp->shp", weight, block_inner, preferred_element_type=jnp.float32
    )
    readout_f = readout.astype(jnp.float32)
    grouped = states.reshape(seq_dev, GROUPS, per_group, half_dim, STATE)
    from_state = jnp.einsum(
        "sgn,sgrpn->sgrp", readout_f, grouped, precision=lax.Precision.HIGHEST
    ).reshape(seq_dev, MIXER_HEADS, half_dim)
    own_score = jnp.repeat(
        jnp.sum(readout_f * conv_input.reshape(seq_dev, GROUPS, STATE), axis=-1), per_group, axis=1
    )
    mix = (
        from_block
        + jnp.exp(total)[:, :, None] * from_state
        + (own_score * step)[:, :, None] * conv_inner
        + skip_gain[None, :, None] * conv_inner
    )
    gated_raw = mix * jax.nn.silu(gate_pre.astype(jnp.float32))
    part_squares = jnp.sum(gated_raw * gated_raw, axis=(1, 2))
    gated = (gated_raw * norm_gain[None]).astype(jnp.bfloat16)
    placed = lax.dynamic_update_slice_in_dim(
        jnp.zeros((seq_all,), jnp.float32), part_squares, own_start, 0
    )
    gate_squares = lax.psum(placed, ("kv", "tp"))
    rms_gate = lax.rsqrt(gate_squares / (MIXER_HEADS * HEAD_DIM) + epsilon)
    by_head = lax.all_to_all(gated, "kv", split_axis=1, concat_axis=0, tiled=True)
    columns = mixer_out
    mixed_full = rms_gate[None, :] * lax.psum(
        jnp.einsum("hpd,shp->ds", columns, by_head, preferred_element_type=jnp.float32),
        ("kv", "tp"),
    )
    mid_full = (whole_f + mixed_full).astype(jnp.bfloat16)
    mid = lax.dynamic_slice_in_dim(mid_full, offset, rows_own, 0)
    full_f = mid_full.astype(jnp.float32)
    mid_squares = jnp.sum(full_f * full_f, axis=0)
    normed_full = (full_f * channel_gain[:, None]).astype(jnp.bfloat16)
    gate_sum = jnp.einsum("ds,df->sf", normed_full, expand_gate, preferred_element_type=jnp.float32)
    value_sum = jnp.einsum(
        "ds,df->sf", normed_full, expand_value, preferred_element_type=jnp.float32
    )
    rms_mid = lax.rsqrt(mid_squares / width + epsilon)
    act = (jax.nn.silu(rms_mid[:, None] * gate_sum) * (rms_mid[:, None] * value_sum)).astype(
        jnp.bfloat16
    )
    columns = reduce_proj
    channel = lax.psum_scatter(
        jnp.einsum("fd,sf->ds", columns, act, preferred_element_type=jnp.float32),
        ("kv", "tp"),
        scatter_dimension=0,
        tiled=True,
    )
    return (mid.astype(jnp.float32) + channel).astype(jnp.bfloat16)


MESH = pl.DeviceIdType.MESH
HIGHEST = lax.Precision.HIGHEST
F32 = jnp.float32
BF16 = jnp.bfloat16


def silu(v):
    return v / (1.0 + jnp.exp(-v))


def rounded(v):
    return v.astype(BF16).astype(F32)


def matmul(a, b):
    return lax.dot_general(a, b, (((1,), (0,)), ((), ())), preferred_element_type=F32)


def matmul_t(a, b):
    return lax.dot_general(a, b, (((1,), (1,)), ((), ())), preferred_element_type=F32)


def matmul_exact(a, b):
    return lax.dot_general(
        a, b, (((1,), (0,)), ((), ())), precision=HIGHEST, preferred_element_type=F32
    )


def layer_kernel(
    kv_n,
    tp_n,
    lengths,
    hidden,
    mixer_gain,
    step_bias,
    decay_log,
    skip_gain,
    taps_inner,
    taps_input,
    taps_output,
    recent_inner,
    recent_input,
    recent_output,
    block_decay,
    norm_gain,
    channel_gain,
    gate_hbm,
    inner_hbm,
    input_hbm,
    output_hbm,
    step_hbm,
    block_input_hbm,
    states_hbm,
    block_inner_hbm,
    mixer_out_hbm,
    expand_gate_hbm,
    expand_value_hbm,
    reduce_hbm,
    out,
    gate_w,
    inner_w,
    input_w,
    output_w,
    step_w,
    block_input,
    states,
    block_inner,
    mixer_out,
    expand_gate,
    expand_value,
    reduce_w,
    head_mask,
    hid_all,
    pre_send,
    pre_recv,
    gated_send,
    gated_recv,
    part_send,
    part_recv,
    mid_send,
    mid_recv,
    last_send,
    last_recv,
    load_sem,
    send_sem,
    recv_sem,
):
    n = kv_n * tp_n
    kv = lax.axis_index("kv")
    tp = lax.axis_index("tp")
    me = kv * tp_n + tp
    seqs, rows = hidden.shape
    half, heads = norm_gain.shape
    groups_n = input_w.shape[1] * kv_n
    state = states.shape[1]
    groups = groups_n // state
    per_group = heads // groups
    span = block_decay.shape[1]
    channels = heads * half
    own_ch = channels // kv_n
    own_in = input_w.shape[1]

    pairs = (
        (output_hbm, output_w),
        (input_hbm, input_w),
        (inner_hbm, inner_w),
        (gate_hbm, gate_w),
        (step_hbm, step_w),
        (block_input_hbm, block_input),
        (states_hbm, states),
        (block_inner_hbm, block_inner),
        (mixer_out_hbm, mixer_out),
        (expand_gate_hbm, expand_gate),
        (expand_value_hbm, expand_value),
        (reduce_hbm, reduce_w),
    )
    loads = {}
    for i, (src, dst) in enumerate(pairs):
        copy = pltpu.make_async_copy(src, dst, load_sem.at[i])
        copy.start()
        loads[id(dst)] = copy

    def loaded(ref):
        loads[id(ref)].wait()
        return ref[...]

    def peer(k):
        other = lax.rem(me + k, n)
        return other, {"kv": other // tp_n, "tp": lax.rem(other, tp_n)}

    barrier = pltpu.get_barrier_semaphore()
    for k in range(1, n):
        pl.semaphore_signal(barrier, inc=1, device_id=peer(k)[1], device_id_type=MESH)
    pl.semaphore_wait(barrier, n - 1)

    pending = []

    def to_all(phase, src_of, dst):
        copies = []
        for k in range(1, n):
            other, where = peer(k)
            copy = pltpu.make_async_remote_copy(
                src_ref=src_of(other),
                dst_ref=dst.at[me],
                send_sem=send_sem.at[phase * n + k],
                recv_sem=recv_sem.at[phase * n + k],
                device_id=where,
                device_id_type=MESH,
            )
            copy.start()
            copies.append(copy)
        pending.extend(copies)
        return copies

    def to_line(phase, src, dst):
        copies = []
        for k in range(1, kv_n):
            other = lax.rem(kv + k, kv_n)
            copy = pltpu.make_async_remote_copy(
                src_ref=src.at[other],
                dst_ref=dst.at[kv],
                send_sem=send_sem.at[phase * n + k],
                recv_sem=recv_sem.at[phase * n + k],
                device_id={"kv": other},
                device_id_type=MESH,
            )
            copy.start()
            copies.append(copy)
        pending.extend(copies)
        return copies

    gather = to_all(0, lambda other: hidden, hid_all)
    hid_all[me] = hidden[...]

    column = lax.broadcasted_iota(jnp.int32, (heads, channels), 1)
    row = lax.broadcasted_iota(jnp.int32, (heads, channels), 0)
    head_mask[...] = jnp.where(
        (column >= row * half) & (column < (row + 1) * half), 1.0, 0.0
    )
    lane = lax.broadcasted_iota(jnp.int32, (half, channels), 1)
    channel = lax.broadcasted_iota(jnp.int32, (half, channels), 0)
    pick = jnp.where(jnp.bitwise_and(lane, half - 1) == channel, 1.0, 0.0)
    window = taps_inner[0] * recent_inner[0].astype(F32)
    for t in range(1, recent_inner.shape[0]):
        window = window + taps_inner[t] * recent_inner[t].astype(F32)
    last = taps_inner.shape[0] - 1

    def spread(a):
        return jnp.sum(pick * matmul_exact(a, head_mask[...]), axis=0, keepdims=True)

    window_row = spread(window)
    tap_row = spread(taps_inner[last])
    norm_row = spread(norm_gain[...])

    def past(taps, recent):
        total = taps[0:1, :] * recent[0:1, :].astype(F32)
        for t in range(1, recent.shape[0]):
            total = total + taps[t : t + 1, :] * recent[t : t + 1, :].astype(F32)
        return total

    past_input = past(taps_input, recent_input)
    past_output = past(taps_output, recent_output)
    diagonal = lax.broadcasted_iota(jnp.int32, (heads, heads), 0) == lax.broadcasted_iota(
        jnp.int32, (heads, heads), 1
    )

    def as_column(v):
        return jnp.sum(jnp.where(diagonal, v, 0.0), axis=1, keepdims=True)

    bias = as_column(step_bias[...])
    rate = jnp.exp(as_column(decay_log[...]))
    skip = as_column(skip_gain[...])
    position = lax.broadcasted_iota(jnp.int32, (1, span), 1)
    live = jnp.where(position < lengths[0], 1.0, 0.0)
    masked = block_decay[...] * live
    cached = jnp.sum(masked, axis=1, keepdims=True)
    later = jnp.where(
        lax.broadcasted_iota(jnp.int32, (span, span), 0)
        > lax.broadcasted_iota(jnp.int32, (span, span), 1),
        1.0,
        0.0,
    )
    suffix = matmul_exact(masked, later)

    for copy in gather:
        copy.wait_recv()
    whole = jnp.concatenate([hid_all[i].astype(F32) for i in range(n)], axis=1)
    rms_in = lax.rsqrt(jnp.mean(whole * whole, axis=1, keepdims=True) + epsilon)
    normed = (whole * mixer_gain[...]).astype(BF16)
    output_part = rounded(rms_in * matmul(normed, loaded(output_w)))
    input_part = rounded(rms_in * matmul(normed, loaded(input_w)))
    inner_part = rounded(rms_in * matmul_t(normed, loaded(inner_w)))
    gate_part = rounded(rms_in * matmul_t(normed, loaded(gate_w)))
    bounds = (0, own_in, 2 * own_in, 2 * own_in + own_ch, 2 * own_in + 2 * own_ch)
    parts = (output_part, input_part, inner_part, gate_part)
    for s in range(seqs):
        for i in range(4):
            pre_send[s, :, bounds[i] : bounds[i + 1]] = parts[i][s : s + 1, :]
    exchange = to_line(1, pre_send, pre_recv)
    pre_recv[kv] = pre_send[kv]

    mine = lax.broadcasted_iota(jnp.int32, (seqs, 1), 0) == kv
    own_rms = jnp.sum(jnp.where(mine, rms_in, 0.0), axis=0, keepdims=True)
    step_all = matmul_t(loaded(step_w), normed)
    mine_lane = lax.broadcasted_iota(jnp.int32, (heads, seqs), 1) == kv
    step_pre = rounded(
        own_rms * jnp.sum(jnp.where(mine_lane, step_all, 0.0), axis=1, keepdims=True)
    )
    v = step_pre + bias
    step = jnp.maximum(v, 0.0) + jnp.log1p(jnp.exp(-jnp.abs(v)))
    new_decay = -rate * step
    kept = live * jnp.exp(new_decay + suffix)
    total = jnp.exp(new_decay + cached)
    states_b = loaded(states).astype(BF16)

    for copy in exchange:
        copy.wait_recv()

    def gathered(i):
        return jnp.concatenate(
            [pre_recv[s, :, bounds[i] : bounds[i + 1]] for s in range(kv_n)], axis=1
        )

    conv_output = rounded(silu(past_output + taps_output[last : last + 1, :] * gathered(0)))
    conv_input = silu(past_input + taps_input[last : last + 1, :] * gathered(1))

    def by_head(v):
        return jnp.concatenate(
            [
                jnp.broadcast_to(v[:, g * state : (g + 1) * state], (per_group, state))
                for g in range(groups)
            ],
            axis=0,
        )

    readout = by_head(conv_output)
    readout_b = readout.astype(BF16)
    own_score = jnp.sum(readout * by_head(conv_input), axis=1, keepdims=True)
    block_in = loaded(block_input)
    score = jnp.concatenate(
        [
            matmul_t(
                readout_b[g * per_group : (g + 1) * per_group, :],
                block_in[:, g * state : (g + 1) * state],
            )
            for g in range(groups)
        ],
        axis=0,
    )
    weight = (kept * score).astype(BF16)
    cross = matmul_t(weight, loaded(block_inner)) + total * matmul_t(readout_b, states_b)
    mask = head_mask[...]
    direct = jnp.sum(mask * (own_score * step + skip), axis=0, keepdims=True)
    conv_inner = silu(window_row + tap_row * gathered(2))
    mix = jnp.sum(mask * cross, axis=0, keepdims=True) + direct * conv_inner
    gated_raw = mix * silu(gathered(3))
    squares = jnp.sum(gated_raw * gated_raw, axis=1, keepdims=True)
    gated = rounded(gated_raw * norm_row)
    tail = gated_send.shape[2] - own_ch
    for s in range(kv_n):
        gated_send[s, :, :own_ch] = gated[:, s * own_ch : (s + 1) * own_ch]
        gated_send[s, :, own_ch:] = jnp.broadcast_to(squares, (1, tail))
    heads_out = to_line(2, gated_send, gated_recv)
    gated_recv[kv] = gated_send[kv]
    out_w = loaded(mixer_out)
    for copy in heads_out:
        copy.wait_recv()
    received = jnp.concatenate([gated_recv[s] for s in range(kv_n)], axis=0)
    partial = matmul(received[:, :own_ch].astype(BF16), out_w)
    for i in range(n):
        part_send[i, :, :rows] = partial[:, i * rows : (i + 1) * rows]
        part_send[i, :, rows:] = received[:, own_ch:]
    reduce_mid = to_all(3, lambda other: part_send.at[other], part_recv)
    part_recv[me] = part_send[me]
    own_hidden = hidden[...].astype(F32)
    for copy in reduce_mid:
        copy.wait_recv()
    summed = part_recv[0]
    for i in range(1, n):
        summed = summed + part_recv[i]
    gate_squares = summed[:, rows : rows + 1] / kv_n
    rms_gate = lax.rsqrt(gate_squares / (channels * tp_n) + epsilon)
    mid = rounded(own_hidden + rms_gate * summed[:, :rows])
    mid_send[...] = mid
    gather_mid = to_all(4, lambda other: mid_send, mid_recv)
    mid_recv[me] = mid
    for copy in gather_mid:
        copy.wait_recv()
    full = jnp.concatenate([mid_recv[i] for i in range(n)], axis=1)
    rms_mid = lax.rsqrt(jnp.mean(full * full, axis=1, keepdims=True) + epsilon)
    normed_mid = (full * channel_gain[...]).astype(BF16)
    gate_sum = rms_mid * matmul_t(normed_mid, loaded(expand_gate))
    value_sum = rms_mid * matmul_t(normed_mid, loaded(expand_value))
    act = (silu(gate_sum) * value_sum).astype(BF16)
    down = matmul(act, loaded(reduce_w))
    for i in range(n):
        last_send[i] = down[:, i * rows : (i + 1) * rows]
    final = to_all(5, lambda other: last_send.at[other], last_recv)
    last_recv[me] = last_send[me]
    for copy in final:
        copy.wait_recv()
    added = last_recv[0]
    for i in range(1, n):
        added = added + last_recv[i]
    out[...] = (mid + added).astype(out.dtype)
    for copy in pending:
        copy.wait_send()


def fused(
    kv_n,
    tp_n,
    hidden,
    mixer_gain,
    gate_proj,
    inner_proj,
    input_proj,
    output_proj,
    step_proj,
    step_bias,
    decay_log,
    skip_gain,
    taps_inner,
    taps_input,
    taps_output,
    recent_inner,
    recent_input,
    recent_output,
    states,
    block_inner,
    block_input,
    block_decay,
    lengths,
    norm_gain,
    mixer_out,
    channel_gain,
    expand_gate,
    expand_value,
    reduce_proj,
):
    rows, seqs = hidden.shape
    width = reduce_proj.shape[1]
    _, heads, half, state = states.shape
    channels = heads * half
    n = kv_n * tp_n
    own_ch = channels // kv_n
    own_in = input_proj.shape[1]
    small = (
        hidden.T,
        mixer_gain[None],
        step_bias[None],
        decay_log[None],
        skip_gain[None],
        taps_inner.transpose(0, 2, 1),
        taps_input,
        taps_output,
        recent_inner[0].transpose(0, 2, 1),
        recent_input[0],
        recent_output[0],
        block_decay[0].T,
        norm_gain.T,
        channel_gain[None],
    )
    large = (
        gate_proj.transpose(1, 2, 0).reshape(own_ch, width),
        inner_proj.transpose(1, 2, 0).reshape(own_ch, width),
        input_proj,
        output_proj,
        step_proj.T,
        block_input[0],
        states.reshape(channels, state),
        block_inner[0].transpose(1, 2, 0).reshape(channels, -1),
        mixer_out.reshape(own_ch, width),
        expand_gate.T,
        expand_value.T,
        reduce_proj,
    )
    pre = 2 * own_in + 2 * own_ch
    result = pl.pallas_call(
        functools.partial(layer_kernel, kv_n, tp_n),
        out_shape=jax.ShapeDtypeStruct((seqs, rows), hidden.dtype),
        in_specs=[pl.BlockSpec(memory_space=pltpu.SMEM)]
        + [pl.BlockSpec(memory_space=pltpu.VMEM)] * len(small)
        + [pl.BlockSpec(memory_space=pl.ANY)] * len(large),
        out_specs=pl.BlockSpec(memory_space=pltpu.VMEM),
        scratch_shapes=[pltpu.VMEM(a.shape, a.dtype) for a in large]
        + [
            pltpu.VMEM((heads, channels), F32),
            pltpu.VMEM((n, seqs, rows), hidden.dtype),
            pltpu.VMEM((kv_n, 1, pre), F32),
            pltpu.VMEM((kv_n, 1, pre), F32),
            pltpu.VMEM((kv_n, 1, own_ch + 128), F32),
            pltpu.VMEM((kv_n, 1, own_ch + 128), F32),
            pltpu.VMEM((n, seqs, rows + 128), F32),
            pltpu.VMEM((n, seqs, rows + 128), F32),
            pltpu.VMEM((seqs, rows), F32),
            pltpu.VMEM((n, seqs, rows), F32),
            pltpu.VMEM((n, seqs, rows), F32),
            pltpu.VMEM((n, seqs, rows), F32),
            pltpu.SemaphoreType.DMA((len(large),)),
            pltpu.SemaphoreType.DMA((6 * n,)),
            pltpu.SemaphoreType.DMA((6 * n,)),
        ],
        compiler_params=pltpu.CompilerParams(
            collective_id=0, has_side_effects=True, vmem_limit_bytes=56 * 1024 * 1024
        ),
    )(lengths, *small, *large)
    return result.T


def wide_enough(kv_n, tp_n, args):
    hidden, input_proj, states = args[0], args[4], args[16]
    rows = hidden.shape[0]
    seq_dev, heads, half, state = states.shape
    return (
        seq_dev == 1
        and hidden.shape[1] == kv_n
        and rows % 128 == 0
        and (heads * half) % (kv_n * 128) == 0
        and input_proj.shape[1] % 128 == 0
        and half & (half - 1) == 0
        and state % 128 == 0
    )


def layer(kv_n, tp_n, *args):
    if wide_enough(kv_n, tp_n, args):
        return fused(kv_n, tp_n, *args)
    return shards(*args)


def solution(mesh):
    return jax.shard_map(
        functools.partial(layer, mesh.shape["kv"], mesh.shape["tp"]),
        mesh=mesh,
        in_specs=(
            P(("kv", "tp"), "dp"),
            P(),
            P(None, "kv", "tp"),
            P(None, "kv", "tp"),
            P(None, "kv"),
            P(None, "kv"),
            P(),
            P(),
            P(),
            P(),
            P(None, None, "tp"),
            P(),
            P(),
            P(("dp", "kv"), None, None, "tp"),
            P(("dp", "kv"), None, None),
            P(("dp", "kv"), None, None),
            P(("dp", "kv"), None, "tp", None),
            P(("dp", "kv"), None, None, "tp"),
            P(("dp", "kv"), None, None),
            P(("dp", "kv"), None, None),
            P(("dp", "kv")),
            P(None, "tp"),
            P("kv", "tp", None),
            P(),
            P(None, ("kv", "tp")),
            P(None, ("kv", "tp")),
            P(("kv", "tp"), None),
        ),
        out_specs=P(("kv", "tp"), "dp"),
        check_vma=False,
    )
```

```python
import jax
import jax.numpy as jnp
from jax import lax
from jax.sharding import PartitionSpec as P
from jax.experimental import pallas as pl
from jax.experimental.pallas import tpu as pltpu
import functools

MIXER_HEADS = 64
HEAD_DIM = 64
GROUPS = 8
STATE = 128
OPEN_BLOCK_SPAN = 128


epsilon = 1e-05


def short_conv(recent, newest, taps):
    window = jnp.concatenate(
        [recent.astype(jnp.float32), newest.astype(jnp.float32)[:, None]], axis=1
    )
    return jax.nn.silu(jnp.sum(window * taps[None], axis=1))


def shards(
    hidden,
    mixer_gain,
    gate_proj,
    inner_proj,
    input_proj,
    output_proj,
    step_proj,
    step_bias,
    decay_log,
    skip_gain,
    taps_inner,
    taps_input,
    taps_output,
    recent_inner,
    recent_input,
    recent_output,
    states,
    block_inner,
    block_input,
    block_decay,
    lengths,
    norm_gain,
    mixer_out,
    channel_gain,
    expand_gate,
    expand_value,
    reduce_proj,
):
    rows_own = hidden.shape[0]
    seq_all = hidden.shape[1]
    seq_dev = states.shape[0]
    half_dim = states.shape[2]
    width = rows_own * lax.axis_size("kv") * lax.axis_size("tp")
    offset = (lax.axis_index("kv") * lax.axis_size("tp") + lax.axis_index("tp")) * rows_own
    own_start = lax.axis_index("kv") * seq_dev
    whole_rows = lax.all_gather(hidden, ("kv", "tp"), axis=0, tiled=True)
    whole_f = whole_rows.astype(jnp.float32)
    rms_in = lax.rsqrt(jnp.mean(whole_f * whole_f, axis=0) + epsilon)
    normed_in = (whole_f * mixer_gain[:, None]).astype(jnp.bfloat16)
    gate_part = (
        rms_in[:, None, None]
        * jnp.einsum("ds,dhp->shp", normed_in, gate_proj, preferred_element_type=jnp.float32)
    ).astype(jnp.bfloat16)
    inner_part = (
        rms_in[:, None, None]
        * jnp.einsum("ds,dhp->shp", normed_in, inner_proj, preferred_element_type=jnp.float32)
    ).astype(jnp.bfloat16)
    input_part = (
        rms_in[:, None]
        * jnp.einsum("ds,dk->sk", normed_in, input_proj, preferred_element_type=jnp.float32)
    ).astype(jnp.bfloat16)
    output_part = (
        rms_in[:, None]
        * jnp.einsum("ds,dk->sk", normed_in, output_proj, preferred_element_type=jnp.float32)
    ).astype(jnp.bfloat16)
    own_cols = lax.dynamic_slice_in_dim(normed_in, own_start, seq_dev, 1)
    own_rms = lax.dynamic_slice_in_dim(rms_in, own_start, seq_dev, 0)
    step_pre = (
        own_rms[:, None]
        * jnp.einsum("ds,dh->sh", own_cols, step_proj, preferred_element_type=jnp.float32)
    ).astype(jnp.bfloat16)
    gate_pre, inner_pre, input_pre, output_pre = (
        lax.all_to_all(gate_part, "kv", split_axis=0, concat_axis=1, tiled=True),
        lax.all_to_all(inner_part, "kv", split_axis=0, concat_axis=1, tiled=True),
        lax.all_to_all(input_part, "kv", split_axis=0, concat_axis=1, tiled=True),
        lax.all_to_all(output_part, "kv", split_axis=0, concat_axis=1, tiled=True),
    )
    conv_inner = short_conv(recent_inner, inner_pre, taps_inner)
    conv_input = short_conv(recent_input, input_pre, taps_input)
    conv_output = short_conv(recent_output, output_pre, taps_output).astype(jnp.bfloat16)
    step = jax.nn.softplus(step_pre.astype(jnp.float32) + step_bias[None, :])
    new_decay = -jnp.exp(decay_log)[None, :] * step
    per_group = MIXER_HEADS // GROUPS
    live = (jnp.arange(OPEN_BLOCK_SPAN, dtype=jnp.int32)[None, :] < lengths[:, None]).astype(
        jnp.float32
    )
    masked = block_decay * live[:, :, None]
    cached = jnp.sum(masked, axis=1)
    tail = new_decay[:, None, :] + cached[:, None, :] - jnp.cumsum(masked, axis=1)
    total = new_decay + cached
    readout = conv_output.reshape(seq_dev, GROUPS, STATE)
    score = jnp.einsum(
        "sgn,sjgn->sgj",
        readout,
        block_input.reshape(seq_dev, OPEN_BLOCK_SPAN, GROUPS, STATE),
        preferred_element_type=jnp.float32,
    )
    score_heads = jnp.repeat(score, per_group, axis=1)
    weight = (live[:, None, :] * jnp.exp(jnp.swapaxes(tail, 1, 2)) * score_heads).astype(
        jnp.bfloat16
    )
    from_block = jnp.einsum(
        "shj,sjhp->shp", weight, block_inner, preferred_element_type=jnp.float32
    )
    readout_f = readout.astype(jnp.float32)
    grouped = states.reshape(seq_dev, GROUPS, per_group, half_dim, STATE)
    from_state = jnp.einsum(
        "sgn,sgrpn->sgrp", readout_f, grouped, precision=lax.Precision.HIGHEST
    ).reshape(seq_dev, MIXER_HEADS, half_dim)
    own_score = jnp.repeat(
        jnp.sum(readout_f * conv_input.reshape(seq_dev, GROUPS, STATE), axis=-1), per_group, axis=1
    )
    mix = (
        from_block
        + jnp.exp(total)[:, :, None] * from_state
        + (own_score * step)[:, :, None] * conv_inner
        + skip_gain[None, :, None] * conv_inner
    )
    gated_raw = mix * jax.nn.silu(gate_pre.astype(jnp.float32))
    part_squares = jnp.sum(gated_raw * gated_raw, axis=(1, 2))
    gated = (gated_raw * norm_gain[None]).astype(jnp.bfloat16)
    placed = lax.dynamic_update_slice_in_dim(
        jnp.zeros((seq_all,), jnp.float32), part_squares, own_start, 0
    )
    gate_squares = lax.psum(placed, ("kv", "tp"))
    rms_gate = lax.rsqrt(gate_squares / (MIXER_HEADS * HEAD_DIM) + epsilon)
    by_head = lax.all_to_all(gated, "kv", split_axis=1, concat_axis=0, tiled=True)
    columns = mixer_out
    mixed_full = rms_gate[None, :] * lax.psum(
        jnp.einsum("hpd,shp->ds", columns, by_head, preferred_element_type=jnp.float32),
        ("kv", "tp"),
    )
    mid_full = (whole_f + mixed_full).astype(jnp.bfloat16)
    mid = lax.dynamic_slice_in_dim(mid_full, offset, rows_own, 0)
    full_f = mid_full.astype(jnp.float32)
    mid_squares = jnp.sum(full_f * full_f, axis=0)
    normed_full = (full_f * channel_gain[:, None]).astype(jnp.bfloat16)
    gate_sum = jnp.einsum("ds,df->sf", normed_full, expand_gate, preferred_element_type=jnp.float32)
    value_sum = jnp.einsum(
        "ds,df->sf", normed_full, expand_value, preferred_element_type=jnp.float32
    )
    rms_mid = lax.rsqrt(mid_squares / width + epsilon)
    act = (jax.nn.silu(rms_mid[:, None] * gate_sum) * (rms_mid[:, None] * value_sum)).astype(
        jnp.bfloat16
    )
    columns = reduce_proj
    channel = lax.psum_scatter(
        jnp.einsum("fd,sf->ds", columns, act, preferred_element_type=jnp.float32),
        ("kv", "tp"),
        scatter_dimension=0,
        tiled=True,
    )
    return (mid.astype(jnp.float32) + channel).astype(jnp.bfloat16)


MESH = pl.DeviceIdType.MESH
HIGHEST = lax.Precision.HIGHEST
F32 = jnp.float32
BF16 = jnp.bfloat16


def silu(v):
    return v / (1.0 + jnp.exp(-v))


def rounded(v):
    return v.astype(BF16).astype(F32)


def matmul(a, b):
    return lax.dot_general(a, b, (((1,), (0,)), ((), ())), preferred_element_type=F32)


def matmul_t(a, b):
    return lax.dot_general(a, b, (((1,), (1,)), ((), ())), preferred_element_type=F32)


def matmul_exact(a, b):
    return lax.dot_general(
        a, b, (((1,), (0,)), ((), ())), precision=HIGHEST, preferred_element_type=F32
    )


def layer_kernel(
    kv_n,
    tp_n,
    lengths_hbm,
    hidden_hbm,
    mixer_gain_hbm,
    step_bias_hbm,
    decay_log_hbm,
    skip_gain_hbm,
    taps_inner_hbm,
    taps_input_hbm,
    taps_output_hbm,
    recent_inner_hbm,
    recent_input_hbm,
    recent_output_hbm,
    block_decay_hbm,
    norm_gain_hbm,
    channel_gain_hbm,
    gate_hbm,
    inner_hbm,
    input_hbm,
    output_hbm,
    step_hbm,
    block_input_hbm,
    states_hbm,
    block_inner_hbm,
    mixer_out_hbm,
    expand_gate_hbm,
    expand_value_hbm,
    reduce_hbm,
    out,
    lengths,
    hidden,
    mixer_gain,
    step_bias,
    decay_log,
    skip_gain,
    taps_inner,
    taps_input,
    taps_output,
    recent_inner,
    recent_input,
    recent_output,
    block_decay,
    norm_gain,
    channel_gain,
    gate_w,
    inner_w,
    input_w,
    output_w,
    step_w,
    block_input,
    states,
    block_inner,
    mixer_out,
    expand_gate,
    expand_value,
    reduce_w,
    head_mask,
    hid_all,
    pre_send,
    pre_recv,
    gated_send,
    gated_recv,
    part_send,
    part_recv,
    mid_send,
    mid_recv,
    last_send,
    last_recv,
    load_sem,
    send_sem,
    recv_sem,
):
    n = kv_n * tp_n
    kv = lax.axis_index("kv")
    tp = lax.axis_index("tp")
    me = kv * tp_n + tp
    seqs, rows = hidden.shape
    half, heads = norm_gain.shape
    groups_n = input_w.shape[1] * kv_n
    state = states.shape[1]
    groups = groups_n // state
    per_group = heads // groups
    span = block_decay.shape[1]
    channels = heads * half
    own_ch = channels // kv_n
    own_in = input_w.shape[1]

    small = (
        (hidden_hbm, hidden),
        (lengths_hbm, lengths),
        (taps_inner_hbm, taps_inner),
        (recent_inner_hbm, recent_inner),
        (norm_gain_hbm, norm_gain),
        (block_decay_hbm, block_decay),
        (taps_input_hbm, taps_input),
        (recent_input_hbm, recent_input),
        (taps_output_hbm, taps_output),
        (recent_output_hbm, recent_output),
        (step_bias_hbm, step_bias),
        (decay_log_hbm, decay_log),
        (skip_gain_hbm, skip_gain),
        (mixer_gain_hbm, mixer_gain),
        (channel_gain_hbm, channel_gain),
    )
    pairs = (
        (output_hbm, output_w),
        (input_hbm, input_w),
        (inner_hbm, inner_w),
        (gate_hbm, gate_w),
        (step_hbm, step_w),
        (block_input_hbm, block_input),
        (states_hbm, states),
        (block_inner_hbm, block_inner),
        (mixer_out_hbm, mixer_out),
        (expand_gate_hbm, expand_gate),
        (expand_value_hbm, expand_value),
        (reduce_hbm, reduce_w),
    )
    loads = {}
    for i, (src, dst) in enumerate(small + pairs):
        copy = pltpu.make_async_copy(src, dst, load_sem.at[i])
        copy.start()
        loads[id(dst)] = copy

    def loaded(ref):
        loads[id(ref)].wait()
        return ref[...]

    def peer(k):
        other = lax.rem(me + k, n)
        return other, {"kv": other // tp_n, "tp": lax.rem(other, tp_n)}

    barrier = pltpu.get_barrier_semaphore()
    for k in range(1, n):
        pl.semaphore_signal(barrier, inc=1, device_id=peer(k)[1], device_id_type=MESH)
    pl.semaphore_wait(barrier, n - 1)

    pending = []

    def to_all(phase, src_of, dst):
        copies = []
        for k in range(1, n):
            other, where = peer(k)
            copy = pltpu.make_async_remote_copy(
                src_ref=src_of(other),
                dst_ref=dst.at[me],
                send_sem=send_sem.at[phase * n + k],
                recv_sem=recv_sem.at[phase * n + k],
                device_id=where,
                device_id_type=MESH,
            )
            copy.start()
            copies.append(copy)
        pending.extend(copies)
        return copies

    def to_line(phase, src, dst):
        copies = []
        for k in range(1, kv_n):
            other = lax.rem(kv + k, kv_n)
            copy = pltpu.make_async_remote_copy(
                src_ref=src.at[other],
                dst_ref=dst.at[kv],
                send_sem=send_sem.at[phase * n + k],
                recv_sem=recv_sem.at[phase * n + k],
                device_id={"kv": other},
                device_id_type=MESH,
            )
            copy.start()
            copies.append(copy)
        pending.extend(copies)
        return copies

    loads[id(hidden)].wait()
    gather = to_all(0, lambda other: hidden, hid_all)
    hid_all[me] = hidden[...]

    for _, ref in small[1:]:
        loads[id(ref)].wait()
    column = lax.broadcasted_iota(jnp.int32, (heads, channels), 1)
    row = lax.broadcasted_iota(jnp.int32, (heads, channels), 0)
    head_mask[...] = jnp.where(
        (column >= row * half) & (column < (row + 1) * half), 1.0, 0.0
    )
    lane = lax.broadcasted_iota(jnp.int32, (half, channels), 1)
    channel = lax.broadcasted_iota(jnp.int32, (half, channels), 0)
    pick = jnp.where(jnp.bitwise_and(lane, half - 1) == channel, 1.0, 0.0)
    window = taps_inner[0] * recent_inner[0].astype(F32)
    for t in range(1, recent_inner.shape[0]):
        window = window + taps_inner[t] * recent_inner[t].astype(F32)
    last = taps_inner.shape[0] - 1

    def spread(a):
        return jnp.sum(pick * matmul_exact(a, head_mask[...]), axis=0, keepdims=True)

    window_row = spread(window)
    tap_row = spread(taps_inner[last])
    norm_row = spread(norm_gain[...])

    def past(taps, recent):
        total = taps[0:1, :] * recent[0:1, :].astype(F32)
        for t in range(1, recent.shape[0]):
            total = total + taps[t : t + 1, :] * recent[t : t + 1, :].astype(F32)
        return total

    past_input = past(taps_input, recent_input)
    past_output = past(taps_output, recent_output)
    diagonal = lax.broadcasted_iota(jnp.int32, (heads, heads), 0) == lax.broadcasted_iota(
        jnp.int32, (heads, heads), 1
    )

    def as_column(v):
        return jnp.sum(jnp.where(diagonal, v, 0.0), axis=1, keepdims=True)

    bias = as_column(step_bias[...])
    rate = jnp.exp(as_column(decay_log[...]))
    skip = as_column(skip_gain[...])
    position = lax.broadcasted_iota(jnp.int32, (1, span), 1)
    live = jnp.where(position < lengths[0], 1.0, 0.0)
    masked = block_decay[...] * live
    cached = jnp.sum(masked, axis=1, keepdims=True)
    later = jnp.where(
        lax.broadcasted_iota(jnp.int32, (span, span), 0)
        > lax.broadcasted_iota(jnp.int32, (span, span), 1),
        1.0,
        0.0,
    )
    suffix = matmul_exact(masked, later)

    for copy in gather:
        copy.wait_recv()
    whole = jnp.concatenate([hid_all[i].astype(F32) for i in range(n)], axis=1)
    rms_in = lax.rsqrt(jnp.mean(whole * whole, axis=1, keepdims=True) + epsilon)
    normed = (whole * mixer_gain[...]).astype(BF16)
    output_part = rounded(rms_in * matmul(normed, loaded(output_w)))
    input_part = rounded(rms_in * matmul(normed, loaded(input_w)))
    inner_part = rounded(rms_in * matmul_t(normed, loaded(inner_w)))
    gate_part = rounded(rms_in * matmul_t(normed, loaded(gate_w)))
    bounds = (0, own_in, 2 * own_in, 2 * own_in + own_ch, 2 * own_in + 2 * own_ch)
    parts = (output_part, input_part, inner_part, gate_part)
    for s in range(seqs):
        for i in range(4):
            pre_send[s, :, bounds[i] : bounds[i + 1]] = parts[i][s : s + 1, :]
    exchange = to_line(1, pre_send, pre_recv)
    pre_recv[kv] = pre_send[kv]

    mine = lax.broadcasted_iota(jnp.int32, (seqs, 1), 0) == kv
    own_rms = jnp.sum(jnp.where(mine, rms_in, 0.0), axis=0, keepdims=True)
    step_all = matmul_t(loaded(step_w), normed)
    mine_lane = lax.broadcasted_iota(jnp.int32, (heads, seqs), 1) == kv
    step_pre = rounded(
        own_rms * jnp.sum(jnp.where(mine_lane, step_all, 0.0), axis=1, keepdims=True)
    )
    v = step_pre + bias
    step = jnp.maximum(v, 0.0) + jnp.log1p(jnp.exp(-jnp.abs(v)))
    new_decay = -rate * step
    kept = live * jnp.exp(new_decay + suffix)
    total = jnp.exp(new_decay + cached)
    states_b = loaded(states).astype(BF16)

    for copy in exchange:
        copy.wait_recv()

    def gathered(i):
        return jnp.concatenate(
            [pre_recv[s, :, bounds[i] : bounds[i + 1]] for s in range(kv_n)], axis=1
        )

    conv_output = rounded(silu(past_output + taps_output[last : last + 1, :] * gathered(0)))
    conv_input = silu(past_input + taps_input[last : last + 1, :] * gathered(1))

    def by_head(v):
        return jnp.concatenate(
            [
                jnp.broadcast_to(v[:, g * state : (g + 1) * state], (per_group, state))
                for g in range(groups)
            ],
            axis=0,
        )

    readout = by_head(conv_output)
    readout_b = readout.astype(BF16)
    own_score = jnp.sum(readout * by_head(conv_input), axis=1, keepdims=True)
    block_in = loaded(block_input)
    score = jnp.concatenate(
        [
            matmul_t(
                readout_b[g * per_group : (g + 1) * per_group, :],
                block_in[:, g * state : (g + 1) * state],
            )
            for g in range(groups)
        ],
        axis=0,
    )
    weight = (kept * score).astype(BF16)
    cross = matmul_t(weight, loaded(block_inner)) + total * matmul_t(readout_b, states_b)
    mask = head_mask[...]
    direct = jnp.sum(mask * (own_score * step + skip), axis=0, keepdims=True)
    conv_inner = silu(window_row + tap_row * gathered(2))
    mix = jnp.sum(mask * cross, axis=0, keepdims=True) + direct * conv_inner
    gated_raw = mix * silu(gathered(3))
    squares = jnp.sum(gated_raw * gated_raw, axis=1, keepdims=True)
    gated = rounded(gated_raw * norm_row)
    tail = gated_send.shape[2] - own_ch
    for s in range(kv_n):
        gated_send[s, :, :own_ch] = gated[:, s * own_ch : (s + 1) * own_ch]
        gated_send[s, :, own_ch:] = jnp.broadcast_to(squares, (1, tail))
    heads_out = to_line(2, gated_send, gated_recv)
    gated_recv[kv] = gated_send[kv]
    out_w = loaded(mixer_out)
    for copy in heads_out:
        copy.wait_recv()
    received = jnp.concatenate([gated_recv[s] for s in range(kv_n)], axis=0)
    partial = matmul(received[:, :own_ch].astype(BF16), out_w)
    for i in range(n):
        part_send[i, :, :rows] = partial[:, i * rows : (i + 1) * rows]
        part_send[i, :, rows:] = received[:, own_ch:]
    reduce_mid = to_all(3, lambda other: part_send.at[other], part_recv)
    part_recv[me] = part_send[me]
    own_hidden = hidden[...].astype(F32)
    for copy in reduce_mid:
        copy.wait_recv()
    summed = part_recv[0]
    for i in range(1, n):
        summed = summed + part_recv[i]
    gate_squares = summed[:, rows : rows + 1] / kv_n
    rms_gate = lax.rsqrt(gate_squares / (channels * tp_n) + epsilon)
    mid = rounded(own_hidden + rms_gate * summed[:, :rows])
    mid_send[...] = mid
    gather_mid = to_all(4, lambda other: mid_send, mid_recv)
    mid_recv[me] = mid
    for copy in gather_mid:
        copy.wait_recv()
    full = jnp.concatenate([mid_recv[i] for i in range(n)], axis=1)
    rms_mid = lax.rsqrt(jnp.mean(full * full, axis=1, keepdims=True) + epsilon)
    normed_mid = (full * channel_gain[...]).astype(BF16)
    gate_sum = rms_mid * matmul_t(normed_mid, loaded(expand_gate))
    value_sum = rms_mid * matmul_t(normed_mid, loaded(expand_value))
    act = (silu(gate_sum) * value_sum).astype(BF16)
    down = matmul(act, loaded(reduce_w))
    for i in range(n):
        last_send[i] = down[:, i * rows : (i + 1) * rows]
    final = to_all(5, lambda other: last_send.at[other], last_recv)
    last_recv[me] = last_send[me]
    for copy in final:
        copy.wait_recv()
    added = last_recv[0]
    for i in range(1, n):
        added = added + last_recv[i]
    out[...] = mid + added
    for copy in pending:
        copy.wait_send()


def fused(
    kv_n,
    tp_n,
    hidden,
    mixer_gain,
    gate_proj,
    inner_proj,
    input_proj,
    output_proj,
    step_proj,
    step_bias,
    decay_log,
    skip_gain,
    taps_inner,
    taps_input,
    taps_output,
    recent_inner,
    recent_input,
    recent_output,
    states,
    block_inner,
    block_input,
    block_decay,
    lengths,
    norm_gain,
    mixer_out,
    channel_gain,
    expand_gate,
    expand_value,
    reduce_proj,
):
    rows, seqs = hidden.shape
    width = reduce_proj.shape[1]
    _, heads, half, state = states.shape
    channels = heads * half
    n = kv_n * tp_n
    own_ch = channels // kv_n
    own_in = input_proj.shape[1]
    small = (
        hidden.T,
        mixer_gain[None],
        step_bias[None],
        decay_log[None],
        skip_gain[None],
        taps_inner.transpose(0, 2, 1),
        taps_input,
        taps_output,
        recent_inner[0].transpose(0, 2, 1),
        recent_input[0],
        recent_output[0],
        block_decay[0].T,
        norm_gain.T,
        channel_gain[None],
    )
    large = (
        gate_proj.transpose(1, 2, 0).reshape(own_ch, width),
        inner_proj.transpose(1, 2, 0).reshape(own_ch, width),
        input_proj,
        output_proj,
        step_proj.T,
        block_input[0],
        states.reshape(channels, state),
        block_inner[0].transpose(1, 2, 0).reshape(channels, -1),
        mixer_out.reshape(own_ch, width),
        expand_gate.T,
        expand_value.T,
        reduce_proj,
    )
    pre = 2 * own_in + 2 * own_ch
    result = pl.pallas_call(
        functools.partial(layer_kernel, kv_n, tp_n),
        out_shape=jax.ShapeDtypeStruct((seqs, rows), F32),
        in_specs=[pl.BlockSpec(memory_space=pl.ANY)] * (1 + len(small) + len(large)),
        out_specs=pl.BlockSpec(memory_space=pltpu.VMEM),
        scratch_shapes=[pltpu.SMEM(lengths.shape, lengths.dtype)]
        + [pltpu.VMEM(a.shape, a.dtype) for a in small + large]
        + [
            pltpu.VMEM((heads, channels), F32),
            pltpu.VMEM((n, seqs, rows), hidden.dtype),
            pltpu.VMEM((kv_n, 1, pre), F32),
            pltpu.VMEM((kv_n, 1, pre), F32),
            pltpu.VMEM((kv_n, 1, own_ch + 128), F32),
            pltpu.VMEM((kv_n, 1, own_ch + 128), F32),
            pltpu.VMEM((n, seqs, rows + 128), F32),
            pltpu.VMEM((n, seqs, rows + 128), F32),
            pltpu.VMEM((seqs, rows), F32),
            pltpu.VMEM((n, seqs, rows), F32),
            pltpu.VMEM((n, seqs, rows), F32),
            pltpu.VMEM((n, seqs, rows), F32),
            pltpu.SemaphoreType.DMA((1 + len(small) + len(large),)),
            pltpu.SemaphoreType.DMA((6 * n,)),
            pltpu.SemaphoreType.DMA((6 * n,)),
        ],
        compiler_params=pltpu.CompilerParams(
            collective_id=0, has_side_effects=True, vmem_limit_bytes=56 * 1024 * 1024
        ),
    )(lengths, *small, *large)
    return result.T.astype(hidden.dtype)


def wide_enough(kv_n, tp_n, args):
    hidden, input_proj, states = args[0], args[4], args[16]
    rows = hidden.shape[0]
    seq_dev, heads, half, state = states.shape
    return (
        seq_dev == 1
        and hidden.shape[1] == kv_n
        and rows % 128 == 0
        and (heads * half) % (kv_n * 128) == 0
        and input_proj.shape[1] % 128 == 0
        and half & (half - 1) == 0
        and state % 128 == 0
    )


def layer(kv_n, tp_n, *args):
    if wide_enough(kv_n, tp_n, args):
        return fused(kv_n, tp_n, *args)
    return shards(*args)


def solution(mesh):
    return jax.shard_map(
        functools.partial(layer, mesh.shape["kv"], mesh.shape["tp"]),
        mesh=mesh,
        in_specs=(
            P(("kv", "tp"), "dp"),
            P(),
            P(None, "kv", "tp"),
            P(None, "kv", "tp"),
            P(None, "kv"),
            P(None, "kv"),
            P(),
            P(),
            P(),
            P(),
            P(None, None, "tp"),
            P(),
            P(),
            P(("dp", "kv"), None, None, "tp"),
            P(("dp", "kv"), None, None),
            P(("dp", "kv"), None, None),
            P(("dp", "kv"), None, "tp", None),
            P(("dp", "kv"), None, None, "tp"),
            P(("dp", "kv"), None, None),
            P(("dp", "kv"), None, None),
            P(("dp", "kv")),
            P(None, "tp"),
            P("kv", "tp", None),
            P(),
            P(None, ("kv", "tp")),
            P(None, ("kv", "tp")),
            P(("kv", "tp"), None),
        ),
        out_specs=P(("kv", "tp"), "dp"),
        check_vma=False,
    )
```

```python
import jax
import jax.numpy as jnp
from jax import lax
from jax.sharding import PartitionSpec as P
from jax.experimental import pallas as pl
from jax.experimental.pallas import tpu as pltpu
import functools

MIXER_HEADS = 64
HEAD_DIM = 64
GROUPS = 8
STATE = 128
OPEN_BLOCK_SPAN = 128


epsilon = 1e-05


def short_conv(recent, newest, taps):
    window = jnp.concatenate(
        [recent.astype(jnp.float32), newest.astype(jnp.float32)[:, None]], axis=1
    )
    return jax.nn.silu(jnp.sum(window * taps[None], axis=1))


def shards(
    hidden,
    mixer_gain,
    gate_proj,
    inner_proj,
    input_proj,
    output_proj,
    step_proj,
    step_bias,
    decay_log,
    skip_gain,
    taps_inner,
    taps_input,
    taps_output,
    recent_inner,
    recent_input,
    recent_output,
    states,
    block_inner,
    block_input,
    block_decay,
    lengths,
    norm_gain,
    mixer_out,
    channel_gain,
    expand_gate,
    expand_value,
    reduce_proj,
):
    rows_own = hidden.shape[0]
    seq_all = hidden.shape[1]
    seq_dev = states.shape[0]
    half_dim = states.shape[2]
    width = rows_own * lax.axis_size("kv") * lax.axis_size("tp")
    offset = (lax.axis_index("kv") * lax.axis_size("tp") + lax.axis_index("tp")) * rows_own
    own_start = lax.axis_index("kv") * seq_dev
    whole_rows = lax.all_gather(hidden, ("kv", "tp"), axis=0, tiled=True)
    whole_f = whole_rows.astype(jnp.float32)
    rms_in = lax.rsqrt(jnp.mean(whole_f * whole_f, axis=0) + epsilon)
    normed_in = (whole_f * mixer_gain[:, None]).astype(jnp.bfloat16)
    gate_part = (
        rms_in[:, None, None]
        * jnp.einsum("ds,dhp->shp", normed_in, gate_proj, preferred_element_type=jnp.float32)
    ).astype(jnp.bfloat16)
    inner_part = (
        rms_in[:, None, None]
        * jnp.einsum("ds,dhp->shp", normed_in, inner_proj, preferred_element_type=jnp.float32)
    ).astype(jnp.bfloat16)
    input_part = (
        rms_in[:, None]
        * jnp.einsum("ds,dk->sk", normed_in, input_proj, preferred_element_type=jnp.float32)
    ).astype(jnp.bfloat16)
    output_part = (
        rms_in[:, None]
        * jnp.einsum("ds,dk->sk", normed_in, output_proj, preferred_element_type=jnp.float32)
    ).astype(jnp.bfloat16)
    own_cols = lax.dynamic_slice_in_dim(normed_in, own_start, seq_dev, 1)
    own_rms = lax.dynamic_slice_in_dim(rms_in, own_start, seq_dev, 0)
    step_pre = (
        own_rms[:, None]
        * jnp.einsum("ds,dh->sh", own_cols, step_proj, preferred_element_type=jnp.float32)
    ).astype(jnp.bfloat16)
    gate_pre, inner_pre, input_pre, output_pre = (
        lax.all_to_all(gate_part, "kv", split_axis=0, concat_axis=1, tiled=True),
        lax.all_to_all(inner_part, "kv", split_axis=0, concat_axis=1, tiled=True),
        lax.all_to_all(input_part, "kv", split_axis=0, concat_axis=1, tiled=True),
        lax.all_to_all(output_part, "kv", split_axis=0, concat_axis=1, tiled=True),
    )
    conv_inner = short_conv(recent_inner, inner_pre, taps_inner)
    conv_input = short_conv(recent_input, input_pre, taps_input)
    conv_output = short_conv(recent_output, output_pre, taps_output).astype(jnp.bfloat16)
    step = jax.nn.softplus(step_pre.astype(jnp.float32) + step_bias[None, :])
    new_decay = -jnp.exp(decay_log)[None, :] * step
    per_group = MIXER_HEADS // GROUPS
    live = (jnp.arange(OPEN_BLOCK_SPAN, dtype=jnp.int32)[None, :] < lengths[:, None]).astype(
        jnp.float32
    )
    masked = block_decay * live[:, :, None]
    cached = jnp.sum(masked, axis=1)
    tail = new_decay[:, None, :] + cached[:, None, :] - jnp.cumsum(masked, axis=1)
    total = new_decay + cached
    readout = conv_output.reshape(seq_dev, GROUPS, STATE)
    score = jnp.einsum(
        "sgn,sjgn->sgj",
        readout,
        block_input.reshape(seq_dev, OPEN_BLOCK_SPAN, GROUPS, STATE),
        preferred_element_type=jnp.float32,
    )
    score_heads = jnp.repeat(score, per_group, axis=1)
    weight = (live[:, None, :] * jnp.exp(jnp.swapaxes(tail, 1, 2)) * score_heads).astype(
        jnp.bfloat16
    )
    from_block = jnp.einsum(
        "shj,sjhp->shp", weight, block_inner, preferred_element_type=jnp.float32
    )
    readout_f = readout.astype(jnp.float32)
    grouped = states.reshape(seq_dev, GROUPS, per_group, half_dim, STATE)
    from_state = jnp.einsum(
        "sgn,sgrpn->sgrp", readout_f, grouped, precision=lax.Precision.HIGHEST
    ).reshape(seq_dev, MIXER_HEADS, half_dim)
    own_score = jnp.repeat(
        jnp.sum(readout_f * conv_input.reshape(seq_dev, GROUPS, STATE), axis=-1), per_group, axis=1
    )
    mix = (
        from_block
        + jnp.exp(total)[:, :, None] * from_state
        + (own_score * step)[:, :, None] * conv_inner
        + skip_gain[None, :, None] * conv_inner
    )
    gated_raw = mix * jax.nn.silu(gate_pre.astype(jnp.float32))
    part_squares = jnp.sum(gated_raw * gated_raw, axis=(1, 2))
    gated = (gated_raw * norm_gain[None]).astype(jnp.bfloat16)
    placed = lax.dynamic_update_slice_in_dim(
        jnp.zeros((seq_all,), jnp.float32), part_squares, own_start, 0
    )
    gate_squares = lax.psum(placed, ("kv", "tp"))
    rms_gate = lax.rsqrt(gate_squares / (MIXER_HEADS * HEAD_DIM) + epsilon)
    by_head = lax.all_to_all(gated, "kv", split_axis=1, concat_axis=0, tiled=True)
    columns = mixer_out
    mixed_full = rms_gate[None, :] * lax.psum(
        jnp.einsum("hpd,shp->ds", columns, by_head, preferred_element_type=jnp.float32),
        ("kv", "tp"),
    )
    mid_full = (whole_f + mixed_full).astype(jnp.bfloat16)
    mid = lax.dynamic_slice_in_dim(mid_full, offset, rows_own, 0)
    full_f = mid_full.astype(jnp.float32)
    mid_squares = jnp.sum(full_f * full_f, axis=0)
    normed_full = (full_f * channel_gain[:, None]).astype(jnp.bfloat16)
    gate_sum = jnp.einsum("ds,df->sf", normed_full, expand_gate, preferred_element_type=jnp.float32)
    value_sum = jnp.einsum(
        "ds,df->sf", normed_full, expand_value, preferred_element_type=jnp.float32
    )
    rms_mid = lax.rsqrt(mid_squares / width + epsilon)
    act = (jax.nn.silu(rms_mid[:, None] * gate_sum) * (rms_mid[:, None] * value_sum)).astype(
        jnp.bfloat16
    )
    columns = reduce_proj
    channel = lax.psum_scatter(
        jnp.einsum("fd,sf->ds", columns, act, preferred_element_type=jnp.float32),
        ("kv", "tp"),
        scatter_dimension=0,
        tiled=True,
    )
    return (mid.astype(jnp.float32) + channel).astype(jnp.bfloat16)


MESH = pl.DeviceIdType.MESH
HIGHEST = lax.Precision.HIGHEST
F32 = jnp.float32
BF16 = jnp.bfloat16


def silu(v):
    return v / (1.0 + jnp.exp(-v))


def rounded(v):
    return v.astype(BF16).astype(F32)


def matmul(a, b):
    return lax.dot_general(a, b, (((1,), (0,)), ((), ())), preferred_element_type=F32)


def matmul_t(a, b):
    return lax.dot_general(a, b, (((1,), (1,)), ((), ())), preferred_element_type=F32)


def matmul_exact(a, b):
    return lax.dot_general(
        a, b, (((1,), (0,)), ((), ())), precision=HIGHEST, preferred_element_type=F32
    )


def layer_kernel(
    kv_n,
    tp_n,
    lengths_hbm,
    hidden_hbm,
    mixer_gain_hbm,
    step_bias_hbm,
    decay_log_hbm,
    skip_gain_hbm,
    taps_inner_hbm,
    taps_input_hbm,
    taps_output_hbm,
    recent_inner_hbm,
    recent_input_hbm,
    recent_output_hbm,
    block_decay_hbm,
    norm_gain_hbm,
    channel_gain_hbm,
    gate_hbm,
    inner_hbm,
    input_hbm,
    output_hbm,
    step_hbm,
    block_input_hbm,
    states_hbm,
    block_inner_hbm,
    mixer_out_hbm,
    expand_gate_hbm,
    expand_value_hbm,
    reduce_hbm,
    out,
    lengths,
    hidden,
    mixer_gain,
    step_bias,
    decay_log,
    skip_gain,
    taps_inner,
    taps_input,
    taps_output,
    recent_inner,
    recent_input,
    recent_output,
    block_decay,
    norm_gain,
    channel_gain,
    gate_w,
    inner_w,
    input_w,
    output_w,
    step_w,
    block_input,
    states,
    block_inner,
    mixer_out,
    expand_gate,
    expand_value,
    reduce_w,
    head_mask,
    hid_all,
    pre_send,
    pre_recv,
    gated_send,
    gated_recv,
    part_send,
    part_recv,
    mid_send,
    mid_recv,
    last_send,
    last_recv,
    load_sem,
    send_sem,
    recv_sem,
):
    n = kv_n * tp_n
    kv = lax.axis_index("kv")
    tp = lax.axis_index("tp")
    me = kv * tp_n + tp
    seqs, rows = hidden.shape
    half, heads = norm_gain.shape
    groups_n = input_w.shape[1] * kv_n
    state = states.shape[1]
    groups = groups_n // state
    per_group = heads // groups
    span = block_decay.shape[1]
    channels = heads * half
    own_ch = channels // kv_n
    own_in = input_w.shape[1]

    small = (
        (hidden_hbm, hidden),
        (lengths_hbm, lengths),
        (taps_inner_hbm, taps_inner),
        (recent_inner_hbm, recent_inner),
        (norm_gain_hbm, norm_gain),
        (block_decay_hbm, block_decay),
        (taps_input_hbm, taps_input),
        (recent_input_hbm, recent_input),
        (taps_output_hbm, taps_output),
        (recent_output_hbm, recent_output),
        (step_bias_hbm, step_bias),
        (decay_log_hbm, decay_log),
        (skip_gain_hbm, skip_gain),
        (mixer_gain_hbm, mixer_gain),
        (channel_gain_hbm, channel_gain),
    )
    pairs = (
        (output_hbm, output_w),
        (input_hbm, input_w),
        (inner_hbm, inner_w),
        (gate_hbm, gate_w),
        (step_hbm, step_w),
        (block_input_hbm, block_input),
        (states_hbm, states),
        (block_inner_hbm, block_inner),
        (mixer_out_hbm, mixer_out),
        (expand_gate_hbm, expand_gate),
        (expand_value_hbm, expand_value),
        (reduce_hbm, reduce_w),
    )
    loads = {}
    for i, (src, dst) in enumerate(small + pairs):
        copy = pltpu.make_async_copy(src, dst, load_sem.at[i])
        copy.start()
        loads[id(dst)] = copy

    def loaded(ref):
        loads[id(ref)].wait()
        return ref[...]

    def peer(k):
        other = lax.rem(me + k, n)
        return other, {"kv": other // tp_n, "tp": lax.rem(other, tp_n)}

    barrier = pltpu.get_barrier_semaphore()
    for k in range(1, n):
        pl.semaphore_signal(barrier, inc=1, device_id=peer(k)[1], device_id_type=MESH)
    pl.semaphore_wait(barrier, n - 1)

    pending = []

    def far_first(k, own, count):
        down = count - 1 - k
        down = down - jnp.where(down <= own, 1, 0)
        up = k + jnp.where(k >= own, 1, 0)
        return jnp.where(2 * own < count, down, up)

    def to_all(phase, src_of, dst):
        copies = []
        for k in range(n - 1):
            other = far_first(k, me, n)
            copy = pltpu.make_async_remote_copy(
                src_ref=src_of(other),
                dst_ref=dst.at[me],
                send_sem=send_sem.at[phase * n + k],
                recv_sem=recv_sem.at[phase * n + me],
                device_id={"kv": other // tp_n, "tp": lax.rem(other, tp_n)},
                device_id_type=MESH,
            )
            copy.start()
            pending.append(copy)
        for k in range(1, n):
            other, where = peer(k)
            copies.append(
                pltpu.make_async_remote_copy(
                    src_ref=src_of(other),
                    dst_ref=dst.at[other],
                    send_sem=send_sem.at[phase * n + k - 1],
                    recv_sem=recv_sem.at[phase * n + other],
                    device_id=where,
                    device_id_type=MESH,
                )
            )
        return copies

    def to_line(phase, src, dst):
        copies = []
        for k in range(1, kv_n):
            other = lax.rem(kv + k, kv_n)
            copy = pltpu.make_async_remote_copy(
                src_ref=src.at[other],
                dst_ref=dst.at[kv],
                send_sem=send_sem.at[phase * n + k],
                recv_sem=recv_sem.at[phase * n + k],
                device_id={"kv": other},
                device_id_type=MESH,
            )
            copy.start()
            copies.append(copy)
        pending.extend(copies)
        return copies

    loads[id(hidden)].wait()
    gather = to_all(0, lambda other: hidden, hid_all)
    hid_all[me] = hidden[...]

    for _, ref in small[1:]:
        loads[id(ref)].wait()
    column = lax.broadcasted_iota(jnp.int32, (heads, channels), 1)
    row = lax.broadcasted_iota(jnp.int32, (heads, channels), 0)
    head_mask[...] = jnp.where(
        (column >= row * half) & (column < (row + 1) * half), 1.0, 0.0
    )
    lane = lax.broadcasted_iota(jnp.int32, (half, channels), 1)
    channel = lax.broadcasted_iota(jnp.int32, (half, channels), 0)
    pick = jnp.where(jnp.bitwise_and(lane, half - 1) == channel, 1.0, 0.0)
    window = taps_inner[0] * recent_inner[0].astype(F32)
    for t in range(1, recent_inner.shape[0]):
        window = window + taps_inner[t] * recent_inner[t].astype(F32)
    last = taps_inner.shape[0] - 1

    def spread(a):
        return jnp.sum(pick * matmul_exact(a, head_mask[...]), axis=0, keepdims=True)

    window_row = spread(window)
    tap_row = spread(taps_inner[last])
    norm_row = spread(norm_gain[...])

    def past(taps, recent):
        total = taps[0:1, :] * recent[0:1, :].astype(F32)
        for t in range(1, recent.shape[0]):
            total = total + taps[t : t + 1, :] * recent[t : t + 1, :].astype(F32)
        return total

    past_input = past(taps_input, recent_input)
    past_output = past(taps_output, recent_output)
    diagonal = lax.broadcasted_iota(jnp.int32, (heads, heads), 0) == lax.broadcasted_iota(
        jnp.int32, (heads, heads), 1
    )

    def as_column(v):
        return jnp.sum(jnp.where(diagonal, v, 0.0), axis=1, keepdims=True)

    bias = as_column(step_bias[...])
    rate = jnp.exp(as_column(decay_log[...]))
    skip = as_column(skip_gain[...])
    position = lax.broadcasted_iota(jnp.int32, (1, span), 1)
    live = jnp.where(position < lengths[0], 1.0, 0.0)
    masked = block_decay[...] * live
    cached = jnp.sum(masked, axis=1, keepdims=True)
    later = jnp.where(
        lax.broadcasted_iota(jnp.int32, (span, span), 0)
        > lax.broadcasted_iota(jnp.int32, (span, span), 1),
        1.0,
        0.0,
    )
    suffix = matmul_exact(masked, later)

    for copy in gather:
        copy.wait_recv()
    whole = jnp.concatenate([hid_all[i].astype(F32) for i in range(n)], axis=1)
    rms_in = lax.rsqrt(jnp.mean(whole * whole, axis=1, keepdims=True) + epsilon)
    normed = (whole * mixer_gain[...]).astype(BF16)
    output_part = rounded(rms_in * matmul(normed, loaded(output_w)))
    input_part = rounded(rms_in * matmul(normed, loaded(input_w)))
    inner_part = rounded(rms_in * matmul_t(normed, loaded(inner_w)))
    gate_part = rounded(rms_in * matmul_t(normed, loaded(gate_w)))
    bounds = (0, own_in, 2 * own_in, 2 * own_in + own_ch, 2 * own_in + 2 * own_ch)
    parts = (output_part, input_part, inner_part, gate_part)
    for s in range(seqs):
        for i in range(4):
            pre_send[s, :, bounds[i] : bounds[i + 1]] = parts[i][s : s + 1, :]
    exchange = to_line(1, pre_send, pre_recv)
    pre_recv[kv] = pre_send[kv]

    mine = lax.broadcasted_iota(jnp.int32, (seqs, 1), 0) == kv
    own_rms = jnp.sum(jnp.where(mine, rms_in, 0.0), axis=0, keepdims=True)
    step_all = matmul_t(loaded(step_w), normed)
    mine_lane = lax.broadcasted_iota(jnp.int32, (heads, seqs), 1) == kv
    step_pre = rounded(
        own_rms * jnp.sum(jnp.where(mine_lane, step_all, 0.0), axis=1, keepdims=True)
    )
    v = step_pre + bias
    step = jnp.maximum(v, 0.0) + jnp.log1p(jnp.exp(-jnp.abs(v)))
    new_decay = -rate * step
    kept = live * jnp.exp(new_decay + suffix)
    total = jnp.exp(new_decay + cached)
    states_b = loaded(states).astype(BF16)

    for copy in exchange:
        copy.wait_recv()

    def gathered(i):
        return jnp.concatenate(
            [pre_recv[s, :, bounds[i] : bounds[i + 1]] for s in range(kv_n)], axis=1
        )

    conv_output = rounded(silu(past_output + taps_output[last : last + 1, :] * gathered(0)))
    conv_input = silu(past_input + taps_input[last : last + 1, :] * gathered(1))

    def by_head(v):
        return jnp.concatenate(
            [
                jnp.broadcast_to(v[:, g * state : (g + 1) * state], (per_group, state))
                for g in range(groups)
            ],
            axis=0,
        )

    readout = by_head(conv_output)
    readout_b = readout.astype(BF16)
    own_score = jnp.sum(readout * by_head(conv_input), axis=1, keepdims=True)
    block_in = loaded(block_input)
    score = jnp.concatenate(
        [
            matmul_t(
                readout_b[g * per_group : (g + 1) * per_group, :],
                block_in[:, g * state : (g + 1) * state],
            )
            for g in range(groups)
        ],
        axis=0,
    )
    weight = (kept * score).astype(BF16)
    cross = matmul_t(weight, loaded(block_inner)) + total * matmul_t(readout_b, states_b)
    mask = head_mask[...]
    direct = jnp.sum(mask * (own_score * step + skip), axis=0, keepdims=True)
    conv_inner = silu(window_row + tap_row * gathered(2))
    mix = jnp.sum(mask * cross, axis=0, keepdims=True) + direct * conv_inner
    gated_raw = mix * silu(gathered(3))
    squares = jnp.sum(gated_raw * gated_raw, axis=1, keepdims=True)
    gated = rounded(gated_raw * norm_row)
    tail = gated_send.shape[2] - own_ch
    for s in range(kv_n):
        gated_send[s, :, :own_ch] = gated[:, s * own_ch : (s + 1) * own_ch]
        gated_send[s, :, own_ch:] = jnp.broadcast_to(squares, (1, tail))
    heads_out = to_line(2, gated_send, gated_recv)
    gated_recv[kv] = gated_send[kv]
    out_w = loaded(mixer_out)
    for copy in heads_out:
        copy.wait_recv()
    received = jnp.concatenate([gated_recv[s] for s in range(kv_n)], axis=0)
    partial = matmul(received[:, :own_ch].astype(BF16), out_w)
    for i in range(n):
        part_send[i, :, :rows] = partial[:, i * rows : (i + 1) * rows]
        part_send[i, :, rows:] = received[:, own_ch:]
    reduce_mid = to_all(3, lambda other: part_send.at[other], part_recv)
    part_recv[me] = part_send[me]
    own_hidden = hidden[...].astype(F32)
    for copy in reduce_mid:
        copy.wait_recv()
    summed = part_recv[0]
    for i in range(1, n):
        summed = summed + part_recv[i]
    gate_squares = summed[:, rows : rows + 1] / kv_n
    rms_gate = lax.rsqrt(gate_squares / (channels * tp_n) + epsilon)
    mid = rounded(own_hidden + rms_gate * summed[:, :rows])
    mid_send[...] = mid
    gather_mid = to_all(4, lambda other: mid_send, mid_recv)
    mid_recv[me] = mid
    for copy in gather_mid:
        copy.wait_recv()
    full = jnp.concatenate([mid_recv[i] for i in range(n)], axis=1)
    rms_mid = lax.rsqrt(jnp.mean(full * full, axis=1, keepdims=True) + epsilon)
    normed_mid = (full * channel_gain[...]).astype(BF16)
    gate_sum = rms_mid * matmul_t(normed_mid, loaded(expand_gate))
    value_sum = rms_mid * matmul_t(normed_mid, loaded(expand_value))
    act = (silu(gate_sum) * value_sum).astype(BF16)
    down = matmul(act, loaded(reduce_w))
    for i in range(n):
        last_send[i] = down[:, i * rows : (i + 1) * rows]
    final = to_all(5, lambda other: last_send.at[other], last_recv)
    last_recv[me] = last_send[me]
    for copy in final:
        copy.wait_recv()
    added = last_recv[0]
    for i in range(1, n):
        added = added + last_recv[i]
    out[...] = mid + added
    for copy in pending:
        copy.wait_send()


def fused(
    kv_n,
    tp_n,
    hidden,
    mixer_gain,
    gate_proj,
    inner_proj,
    input_proj,
    output_proj,
    step_proj,
    step_bias,
    decay_log,
    skip_gain,
    taps_inner,
    taps_input,
    taps_output,
    recent_inner,
    recent_input,
    recent_output,
    states,
    block_inner,
    block_input,
    block_decay,
    lengths,
    norm_gain,
    mixer_out,
    channel_gain,
    expand_gate,
    expand_value,
    reduce_proj,
):
    rows, seqs = hidden.shape
    width = reduce_proj.shape[1]
    _, heads, half, state = states.shape
    channels = heads * half
    n = kv_n * tp_n
    own_ch = channels // kv_n
    own_in = input_proj.shape[1]
    small = (
        hidden.T,
        mixer_gain[None],
        step_bias[None],
        decay_log[None],
        skip_gain[None],
        taps_inner.transpose(0, 2, 1),
        taps_input,
        taps_output,
        recent_inner[0].transpose(0, 2, 1),
        recent_input[0],
        recent_output[0],
        block_decay[0].T,
        norm_gain.T,
        channel_gain[None],
    )
    large = (
        gate_proj.transpose(1, 2, 0).reshape(own_ch, width),
        inner_proj.transpose(1, 2, 0).reshape(own_ch, width),
        input_proj,
        output_proj,
        step_proj.T,
        block_input[0],
        states.reshape(channels, state),
        block_inner[0].transpose(1, 2, 0).reshape(channels, -1),
        mixer_out.reshape(own_ch, width),
        expand_gate.T,
        expand_value.T,
        reduce_proj,
    )
    pre = 2 * own_in + 2 * own_ch
    result = pl.pallas_call(
        functools.partial(layer_kernel, kv_n, tp_n),
        out_shape=jax.ShapeDtypeStruct((seqs, rows), F32),
        in_specs=[pl.BlockSpec(memory_space=pl.ANY)] * (1 + len(small) + len(large)),
        out_specs=pl.BlockSpec(memory_space=pltpu.VMEM),
        scratch_shapes=[pltpu.SMEM(lengths.shape, lengths.dtype)]
        + [pltpu.VMEM(a.shape, a.dtype) for a in small + large]
        + [
            pltpu.VMEM((heads, channels), F32),
            pltpu.VMEM((n, seqs, rows), hidden.dtype),
            pltpu.VMEM((kv_n, 1, pre), F32),
            pltpu.VMEM((kv_n, 1, pre), F32),
            pltpu.VMEM((kv_n, 1, own_ch + 128), F32),
            pltpu.VMEM((kv_n, 1, own_ch + 128), F32),
            pltpu.VMEM((n, seqs, rows + 128), F32),
            pltpu.VMEM((n, seqs, rows + 128), F32),
            pltpu.VMEM((seqs, rows), F32),
            pltpu.VMEM((n, seqs, rows), F32),
            pltpu.VMEM((n, seqs, rows), F32),
            pltpu.VMEM((n, seqs, rows), F32),
            pltpu.SemaphoreType.DMA((1 + len(small) + len(large),)),
            pltpu.SemaphoreType.DMA((6 * n,)),
            pltpu.SemaphoreType.DMA((6 * n,)),
        ],
        compiler_params=pltpu.CompilerParams(
            collective_id=0, has_side_effects=True, vmem_limit_bytes=56 * 1024 * 1024
        ),
    )(lengths, *small, *large)
    return result.T.astype(hidden.dtype)


def wide_enough(kv_n, tp_n, args):
    hidden, input_proj, states = args[0], args[4], args[16]
    rows = hidden.shape[0]
    seq_dev, heads, half, state = states.shape
    return (
        seq_dev == 1
        and hidden.shape[1] == kv_n
        and rows % 128 == 0
        and (heads * half) % (kv_n * 128) == 0
        and input_proj.shape[1] % 128 == 0
        and half & (half - 1) == 0
        and state % 128 == 0
    )


def layer(kv_n, tp_n, *args):
    if wide_enough(kv_n, tp_n, args):
        return fused(kv_n, tp_n, *args)
    return shards(*args)


def solution(mesh):
    return jax.shard_map(
        functools.partial(layer, mesh.shape["kv"], mesh.shape["tp"]),
        mesh=mesh,
        in_specs=(
            P(("kv", "tp"), "dp"),
            P(),
            P(None, "kv", "tp"),
            P(None, "kv", "tp"),
            P(None, "kv"),
            P(None, "kv"),
            P(),
            P(),
            P(),
            P(),
            P(None, None, "tp"),
            P(),
            P(),
            P(("dp", "kv"), None, None, "tp"),
            P(("dp", "kv"), None, None),
            P(("dp", "kv"), None, None),
            P(("dp", "kv"), None, "tp", None),
            P(("dp", "kv"), None, None, "tp"),
            P(("dp", "kv"), None, None),
            P(("dp", "kv"), None, None),
            P(("dp", "kv")),
            P(None, "tp"),
            P("kv", "tp", None),
            P(),
            P(None, ("kv", "tp")),
            P(None, ("kv", "tp")),
            P(("kv", "tp"), None),
        ),
        out_specs=P(("kv", "tp"), "dp"),
        check_vma=False,
    )
```
